32 devices in a mesh: sp: 8 (over z, core), tp: 4 (over y, x).
Axes of the slice: x: 2, y: 2, z: 4, core: 2. Of those that a mesh axis runs over, the one named last changes fastest.
Arguments:
- residual_signal: bfloat16 [1024, 2048], P(('sp', 'tp')), may hold values from -6 to 6
- prelayer_scaling_factor: float32 [2048], replicated, may hold values from 0.1 to 1.9
- result_adjoint: bfloat16 [1024, 2048], P(('sp', 'tp')), may hold values from -12 to 12
- chosen_specialist_ids: int32 [1024, 2], P('sp'), may hold values from 0 to 7, all different within a row; in each aligned block of 128 rows (0 to 127, 128 to 255, ...) at most 40 rows name the same one
- dispatch_shares: float32 [1024, 2], P('sp'), may hold values from 0.2 to 1
- specialist_valve_matrix: bfloat16 [8, 2048, 2048], P('sp', None, 'tp'), may hold values from -0.125 to 0.125
- specialist_widen_matrix: bfloat16 [8, 2048, 2048], P('sp', None, 'tp'), may hold values from -0.125 to 0.125
- specialist_shrink_matrix: bfloat16 [8, 2048, 2048], P('sp', 'tp'), may hold values from -0.125 to 0.125
- probe_vectors: bfloat16 [1024, 1024], P('sp'), may hold values from -6 to 6
- lookup_vectors: bfloat16 [1024, 1024], P('sp'), may hold values from -1.5 to 1.5
- persistence_scores: bfloat16 [1024, 1024], P('sp'), may hold values from -2 to 8
- group_additional_shrinkage: float32 [1024, 2], P('sp'), may hold values from -4.2 to 0
- content_vectors: bfloat16 [1024, 2, 1024], P('sp', None, 'tp'), may hold values from -6 to 6
- result_valve_scores: bfloat16 [1024, 2, 1024], P('sp', None, 'tp'), may hold values from -6 to 6
- stored_opening_memory: float32 [8, 2, 512, 1024], P('sp', None, None, 'tp'), may hold values from -24 to 24
- result_mapping_matrix: bfloat16 [2048, 2, 1024], P(None, None, 'tp'), may hold values from -0.125 to 0.125
Outputs:
- stream_grad: bfloat16 [1024, 2048], P(('sp', 'tp'))
- gate_grad: bfloat16 [8, 2048, 2048], P('sp', None, 'tp')
- up_grad: bfloat16 [8, 2048, 2048], P('sp', None, 'tp')
- down_grad: bfloat16 [8, 2048, 2048], P('sp', 'tp')
- proj_grad: float32 [2048, 2, 1024], P('sp', None, 'tp')
- query_grad: bfloat16 [1024, 1024], P('sp', 'tp')
- key_grad: bfloat16 [1024, 1024], P('sp', 'tp')
- retain_preact_derivative: float32 [1024, 1024], P('sp', 'tp')
- value_grad: bfloat16 [1024, 2, 1024], P('sp', None, 'tp')
- gate_input_grad: bfloat16 [1024, 2, 1024], P('sp', None, 'tp')
The draws below stay inside these ranges and needn't reach their ends.
Inputs may be any that keep to these rules, and one draw needn't show every extreme that they name: `chosen_specialist_ids`: the 2 experts of a token differ. In each aligned block of 128 tokens no expert is named by more than 40 tokens, a bound that some expert reaches in some block.
All inputs are finite; a program needn't handle non-finite values.
Results may differ from the reference program's by a relative error of at most 0.028.
Values may be sent and summed in bfloat16 or wider, within the bound.
No kernel may reach another device: no remote copies, remote signals or barrier semaphores. Data moves between devices by JAX's collectives and lax.ppermute only.
A program may use at most 64 MiB of HBM per device.

```python
import math
import jax
import jax.numpy as jnp
import numpy as np
from jax import lax

D = 2048
FOCUS_GROUPS = 2
FEATURE_DIMS = 512
HEAD_V = 1024
FF = 2048
TOP = 2
PIECE_PLACES = 64
TOK_DEV = 128
CORPUS_SPAN = 1024
EXPERTS = 8
QUERY_CHANNELS = 1024
CAP = 40
FF_PART = 512
HV_PART = 256
N_SP = 8
N_TP = 4


def draw_persistence_scores(key, part):
    channel_count = FOCUS_GROUPS * FEATURE_DIMS
    pick_key, fast_key, span_key, noise_key = jax.random.split(jax.random.fold_in(key, 11), 4)
    picks = jax.random.randint(pick_key, (channel_count,), 0, 20)
    slow_mask = picks < 10
    slow_level = jnp.log(jnp.float32(CORPUS_SPAN) / 25.6)
    fast_level = jax.random.uniform(fast_key, (channel_count,), jnp.float32, -0.5, 1.0)
    levels = jnp.where(slow_mask, slow_level, fast_level)
    span_shift = jnp.repeat(jax.random.uniform(span_key, (CORPUS_SPAN // TOK_DEV, 1), jnp.float32, -0.5, 0.5), TOK_DEV, axis=0)
    noise = jax.random.uniform(noise_key, (CORPUS_SPAN, channel_count), jnp.float32, -1.0, 1.0)
    return (levels[None, :] + span_shift + noise).astype(jnp.bfloat16)


def draw_group_additional_shrinkage(key, part):
    place_key, loss_key = jax.random.split(jax.random.fold_in(key, 23))
    places = jax.random.randint(place_key, (FOCUS_GROUPS, 6), 0, CORPUS_SPAN)
    losses = jax.random.uniform(loss_key, (FOCUS_GROUPS, 6), jnp.float32, 0.2, 0.5)
    hits = jnp.arange(CORPUS_SPAN, dtype=jnp.int32)[:, None, None] == places[None, :, :]
    return jnp.sum(jnp.where(hits, jnp.log(1.0 - losses)[None], 0.0), axis=2).astype(jnp.float32)


def raised(array, rng, source, target, blocks, factor):
    def block_of(axis_at):
        return (jnp.arange(array.shape[axis_at]) // (array.shape[axis_at] // blocks)).reshape((-1,) + (1,) * (array.ndim - 1 - axis_at))

    first = jax.random.permutation(rng, blocks)[block_of(target)]
    other_side = (block_of(target) + blocks // 2) % blocks
    return jnp.where((block_of(source) == first) | (block_of(source) == other_side), factor * array, array)


def block_scale(key, extent, cuts, smallest, top_value):
    def one(dim, parts):
        steps = jax.random.uniform(jax.random.fold_in(jax.random.fold_in(key, 6), dim), (parts,), jnp.float32, smallest / len(cuts), top_value / len(cuts))
        return jnp.repeat(jnp.exp(steps), extent[dim] // parts).reshape((-1,) + (1,) * (len(extent) - dim - 1))

    gain = one(*cuts[0])
    for cut in cuts[1:]:
        gain = gain * one(*cut)
    return gain


def routed_block(own_key, own, number, rows, number_of, top, bound, skew):
    sequence = jax.random.permutation(own_key, number_of)
    crowded, ordinary = portions_of(number_of, rows * top, bound, skew, True), portions_of(number_of, rows * top, bound, skew, False)
    places = jnp.arange(number_of)

    def named(tallies, turn):
        used = int((tallies > 0).sum())
        fixed = max(1, used // 4)
        moved = fixed + (places - fixed + turn * (used - fixed)) % max(1, number_of - fixed)
        return jnp.zeros((number_of,), jnp.int32).at[sequence[jnp.where(places < fixed, places, moved)]].set(jnp.asarray(tallies, jnp.int32))

    tallies = jnp.where(number % 4 == 0, named(crowded, number // 4), named(ordinary, number - number // 4 - 1))
    mixed = jax.random.permutation(jax.random.fold_in(own, 3), number_of)
    donor, taker = mixed[0:number_of // 2 * 2:2], mixed[1:number_of // 2 * 2:2]
    room = jnp.minimum(tallies[donor] - 1, bound - tallies[taker]) // 2
    room = jnp.where((donor == sequence[0]) | (taker == sequence[0]) | (tallies[taker] == 0), 0, jnp.maximum(room, 0))
    moved = jax.random.randint(jax.random.fold_in(own, 4), (number_of // 2,), 0, 1 << 20) % (room + 1)
    tallies = tallies.at[donor].add(-moved).at[taker].add(moved)
    labels = jnp.searchsorted(jnp.cumsum(tallies), jnp.arange(rows * top), side="right").astype(jnp.int32)
    table = labels.reshape(top, rows).T
    table = table[jax.random.permutation(jax.random.fold_in(own, 1), rows)]
    turn = jax.random.randint(jax.random.fold_in(own, 2), (rows, 1), 0, top)
    return jnp.take_along_axis(table, (jnp.arange(top)[None, :] + turn) % top, axis=1)


def portions_of(count, total, most, slope, full):
    portions = [(1 << 20) // math.isqrt(standing ** slope) + 1 for standing in range(1, count + 1)]
    largest = most if full else min(most, max(-(-total // count), total * portions[0] // sum(portions)))
    least = 1 if total - largest >= count - 1 else 0
    given, surplus = [largest] + [least] * (count - 1), total - largest - least * (count - 1)
    while surplus > 0:
        movable = [i for i in range(1, count) if given[i] < largest] or [i for i in range(1, count) if given[i] < most]
        whole, budget = sum([portions[i] for i in movable]), surplus
        for i in movable:
            extra = min(most - given[i], max(1, budget * portions[i] // whole), surplus)
            given[i] = given[i] + extra
            surplus = surplus - extra
    return np.array(given)


def bell_draw(key, extent, scale, reach, cuts=(), held_as=jnp.bfloat16):
    drawn = jax.random.normal(key, extent, jnp.float32) * scale
    if len(cuts) > 0:
        drawn = block_scale(key, extent, cuts, -0.22, 0.18) * drawn
    return jnp.clip(drawn, min=-reach, max=reach).astype(held_as)


def gaussian_with(rng, dims, scale, reach, pieces, heavy, kind=jnp.bfloat16):
    drawn = scale * jax.random.normal(rng, dims, jnp.float32)
    if pieces:
        drawn = drawn * block_scale(rng, dims, pieces, -0.22, 0.18)
    return jnp.clip(raised(drawn, jax.random.fold_in(rng, 3), *heavy), -reach, reach).astype(kind)


def setup_inputs(seed: int = 0) -> dict:
    key_of = jax.random.split(jax.random.key(seed), 17)
    residual_signal = bell_draw(key_of[0], (CORPUS_SPAN, D), 1.0, 6.0, ((0, 32),))
    prelayer_scaling_factor = jnp.clip(1.0 + 0.18 * jax.random.normal(key_of[1], (D,), jnp.float32), 0.1, 1.9)
    result_adjoint = gaussian_with(key_of[2], (CORPUS_SPAN, D), 1.0, 12.0, ((0, 32),), (0, 1, 32, 2.75))
    chosen_specialist_ids_keys = jax.random.split(jax.random.fold_in(key_of[3], 1), CORPUS_SPAN // TOK_DEV)
    chosen_specialist_ids_turns = jax.random.permutation(jax.random.fold_in(key_of[3], 3), CORPUS_SPAN // TOK_DEV)
    chosen_specialist_ids = jax.vmap(lambda own, number: routed_block(jax.random.fold_in(key_of[3], 2), own, number, TOK_DEV, EXPERTS, TOP, CAP, 2))(chosen_specialist_ids_keys, chosen_specialist_ids_turns).reshape((CORPUS_SPAN, TOP))
    dispatch_shares = jnp.clip(0.2 + 0.8 * jax.random.uniform(key_of[4], (CORPUS_SPAN, TOP), jnp.float32) ** block_scale(key_of[4], (CORPUS_SPAN, TOP), ((0, 8),), -0.2, 0.2), 0.2, 1.0)
    specialist_valve_matrix = bell_draw(key_of[5], (EXPERTS, D, FF), D ** -0.5, 0.125, ((0, 8), (2, 4)))
    specialist_widen_matrix = bell_draw(key_of[6], (EXPERTS, D, FF), D ** -0.5, 0.125, ((0, 8), (2, 4)))
    specialist_shrink_matrix = bell_draw(key_of[7], (EXPERTS, FF, D), FF ** -0.5, 0.125, ((0, 8), (1, 4)))
    probe_vectors = bell_draw(key_of[8], (CORPUS_SPAN, QUERY_CHANNELS), 1.0, 6.0, ((0, 8),))
    lookup_vectors = bell_draw(key_of[9], (CORPUS_SPAN, QUERY_CHANNELS), 0.25, 1.5, ((0, 8),))
    persistence_scores = draw_persistence_scores(jax.random.fold_in(key_of[16], 71), 0)
    group_additional_shrinkage = draw_group_additional_shrinkage(jax.random.fold_in(key_of[16], 71), 0)
    content_vectors = bell_draw(key_of[12], (CORPUS_SPAN, FOCUS_GROUPS, HEAD_V), 1.0, 6.0, ((0, 8), (2, 4)))
    result_valve_scores = bell_draw(key_of[13], (CORPUS_SPAN, FOCUS_GROUPS, HEAD_V), 1.0, 6.0, ((0, 8), (2, 4)))
    stored_opening_memory = bell_draw(key_of[14], (N_SP, FOCUS_GROUPS, FEATURE_DIMS, HEAD_V), 4.0, 24.0, ((0, 8), (3, 4)), jnp.float32)
    result_mapping_matrix = bell_draw(key_of[15], (D, FOCUS_GROUPS, HEAD_V), (FOCUS_GROUPS * HEAD_V) ** -0.5, 0.125, ((2, 4),))
    return {"residual_signal": residual_signal, "prelayer_scaling_factor": prelayer_scaling_factor, "result_adjoint": result_adjoint, "chosen_specialist_ids": chosen_specialist_ids, "dispatch_shares": dispatch_shares, "specialist_valve_matrix": specialist_valve_matrix, "specialist_widen_matrix": specialist_widen_matrix, "specialist_shrink_matrix": specialist_shrink_matrix, "probe_vectors": probe_vectors, "lookup_vectors": lookup_vectors, "persistence_scores": persistence_scores, "group_additional_shrinkage": group_additional_shrinkage, "content_vectors": content_vectors, "result_valve_scores": result_valve_scores, "stored_opening_memory": stored_opening_memory, "result_mapping_matrix": result_mapping_matrix}


toggle_smoothness = 16.0
norm_eps = 1e-06

def silu_slope(value):
    sigma = jax.nn.sigmoid(value)
    return sigma + value * sigma * (1.0 - sigma)

def expert_rows(item, input_rows, cot_rows):
    w_gate, w_up, w_down, index = item
    inputs = input_rows[index]
    cotangent = cot_rows[index]
    contract_last = (((1,), (1,)), ((), ()))
    contract_first = (((0,), (0,)), ((), ()))
    pre_gate = jnp.dot(inputs, w_gate, preferred_element_type=jnp.float32)
    pre_up = jnp.dot(inputs, w_up, preferred_element_type=jnp.float32)
    hidden = (jax.nn.silu(pre_gate) * pre_up).astype(jnp.bfloat16)
    hidden_grad = lax.dot_general(cotangent, w_down, contract_last, preferred_element_type=jnp.float32)
    down_part = lax.dot_general(hidden, cotangent, contract_first, preferred_element_type=jnp.float32).astype(jnp.bfloat16)
    gate_pre = (hidden_grad * pre_up * silu_slope(pre_gate)).astype(jnp.bfloat16)
    up_pre = (hidden_grad * jax.nn.silu(pre_gate)).astype(jnp.bfloat16)
    gate_part = lax.dot_general(inputs, gate_pre, contract_first, preferred_element_type=jnp.float32).astype(jnp.bfloat16)
    up_part = lax.dot_general(inputs, up_pre, contract_first, preferred_element_type=jnp.float32).astype(jnp.bfloat16)
    row_count = inputs.shape[0]
    group_gate = gate_pre.astype(jnp.float32).reshape(row_count, N_TP, FF_PART)
    group_up = up_pre.astype(jnp.float32).reshape(row_count, N_TP, FF_PART)
    weight_gate = w_gate.astype(jnp.float32).reshape(D, N_TP, FF_PART)
    weight_up = w_up.astype(jnp.float32).reshape(D, N_TP, FF_PART)
    groups = jnp.einsum('rgf,dgf->grd', group_gate, weight_gate) + jnp.einsum('rgf,dgf->grd', group_up, weight_up)
    groups = lax.optimization_barrier(groups.astype(jnp.bfloat16))
    routed = lax.optimization_barrier(jnp.sum(groups.astype(jnp.float32), axis=0)).astype(jnp.bfloat16)
    return (routed, gate_part, up_part, down_part)

def reference(residual_signal, prelayer_scaling_factor, result_adjoint, chosen_specialist_ids, dispatch_shares, specialist_valve_matrix, specialist_widen_matrix, specialist_shrink_matrix, probe_vectors, lookup_vectors, persistence_scores, group_additional_shrinkage, content_vectors, result_valve_scores, stored_opening_memory, result_mapping_matrix):
    residual = residual_signal.astype(jnp.float32)
    inv_rms = lax.rsqrt(lax.optimization_barrier(jnp.mean(residual * residual, axis=1, keepdims=True)) + norm_eps)
    unit_rows = residual * inv_rms
    moe_input = (unit_rows * prelayer_scaling_factor).astype(jnp.bfloat16)
    weighted = (dispatch_shares[:, :, None] * result_adjoint.astype(jnp.float32)[:, None, :]).astype(jnp.bfloat16)
    span_ids = chosen_specialist_ids.reshape(N_SP, TOK_DEV * TOP)
    one_hot = (span_ids[:, :, None] == jnp.arange(EXPERTS, dtype=jnp.int32)[None, None, :]).astype(jnp.int32)
    slot_index = lax.optimization_barrier(jnp.sum((jnp.cumsum(one_hot, axis=1) - one_hot) * one_hot, axis=2))
    span_index = jnp.arange(N_SP, dtype=jnp.int32)[:, None]
    destination = (span_ids * (N_SP * CAP) + span_index * CAP + slot_index).reshape(-1)
    assigned = CORPUS_SPAN * TOP
    source_of = jnp.full((EXPERTS * N_SP * CAP,), assigned, jnp.int32).at[destination].set(jnp.arange(assigned, dtype=jnp.int32))
    zero_row = jnp.zeros((1, D), jnp.bfloat16)
    input_rows = jnp.concatenate([jnp.repeat(moe_input, TOP, axis=0), zero_row], axis=0)
    cot_rows = jnp.concatenate([weighted.reshape(assigned, D), zero_row], axis=0)
    routed, gate_grad, up_grad, down_grad = lax.map(lambda item: expert_rows(item, input_rows, cot_rows), (specialist_valve_matrix, specialist_widen_matrix, specialist_shrink_matrix, source_of.reshape(EXPERTS, N_SP * CAP)))
    picked = routed.reshape(EXPERTS * N_SP * CAP, D)[destination].astype(jnp.float32)
    input_grad = lax.optimization_barrier(jnp.sum(picked.reshape(CORPUS_SPAN, TOP, D), axis=1))
    scaled = prelayer_scaling_factor * input_grad
    stream_full = result_adjoint.astype(jnp.float32) + inv_rms * (scaled - unit_rows * lax.optimization_barrier(jnp.mean(scaled * unit_rows, axis=1, keepdims=True)))
    stream_grad = stream_full.astype(jnp.bfloat16)
    piece_ordinal = CORPUS_SPAN // PIECE_PLACES
    per_span = TOK_DEV // PIECE_PLACES
    query_scale = FEATURE_DIMS ** (-0.5)
    exponent_shrinkage = (jax.nn.log_sigmoid(persistence_scores.astype(jnp.float32)).reshape(CORPUS_SPAN, FOCUS_GROUPS, FEATURE_DIMS) / toggle_smoothness + group_additional_shrinkage[:, :, None]).reshape(piece_ordinal, PIECE_PLACES, FOCUS_GROUPS, FEATURE_DIMS)
    cumulative = jnp.cumsum(exponent_shrinkage, axis=1)
    totals = cumulative[:, -1]
    factor = jnp.exp(totals[:, None] - cumulative)
    key_weight = lookup_vectors.astype(jnp.float32).reshape(piece_ordinal, PIECE_PLACES, FOCUS_GROUPS, FEATURE_DIMS) * factor
    decayed = key_weight.astype(jnp.bfloat16)
    value_blocks = content_vectors.astype(jnp.float32).reshape(piece_ordinal, PIECE_PLACES, FOCUS_GROUPS, HEAD_V)
    scaled_query = probe_vectors.astype(jnp.float32).reshape(piece_ordinal, PIECE_PLACES, FOCUS_GROUPS, FEATURE_DIMS) * query_scale

    def to_spans(tensor):
        return tensor.reshape((N_SP, per_span) + tensor.shape[1:])

    def span_states(item):
        begin_state, span_totals, span_decayed, span_values = item

        def block_step(running_state, inputs):
            total_of_block, decayed_block_terms, value_rows_block = inputs
            updated_state = running_state * jnp.exp(total_of_block)[:, :, None] + jnp.einsum('yno,ynt->not', decayed_block_terms.astype(jnp.float32), value_rows_block)
            return (updated_state, (running_state, updated_state))
        unused, pair = lax.scan(block_step, begin_state, (span_totals, span_decayed, span_values))
        return pair
    priors, states = lax.map(span_states, (stored_opening_memory, to_spans(totals), to_spans(decayed), to_spans(value_blocks)))
    priors = priors.reshape(piece_ordinal, FOCUS_GROUPS, FEATURE_DIMS, HEAD_V)
    states = states.reshape(piece_ordinal, FOCUS_GROUPS, FEATURE_DIMS, HEAD_V)
    readout = jnp.einsum('bchk,bhkv->bchv', scaled_query, states).reshape(CORPUS_SPAN, FOCUS_GROUPS, HEAD_V)
    gated_grad = jnp.einsum('td,dhv->thv', stream_grad.astype(jnp.float32), result_mapping_matrix.astype(jnp.float32))
    gate_value = result_valve_scores.astype(jnp.float32)
    gate_silu = jax.nn.silu(gate_value)
    gated_rows = (readout * gate_silu).astype(jnp.bfloat16)
    proj_grad = jnp.einsum('td,thv->dhv', stream_grad.astype(jnp.float32), gated_rows.astype(jnp.float32))
    readout_grad = gated_grad * gate_silu
    gate_input_grad = (gated_grad * readout * silu_slope(gate_value)).astype(jnp.bfloat16)
    readout_blocks = readout_grad.reshape(piece_ordinal, PIECE_PLACES, FOCUS_GROUPS, HEAD_V)
    local_terms = jnp.einsum('bchk,bchv->bhkv', scaled_query, readout_blocks)

    def back_step(carried, inputs):
        block_local, total_of_block = inputs
        block_grad = block_local + carried
        return (block_grad * jnp.exp(total_of_block)[:, :, None], block_grad)
    unused, state_grad = lax.scan(back_step, jnp.zeros((FOCUS_GROUPS, FEATURE_DIMS, HEAD_V), jnp.float32), (local_terms, totals), reverse=True)
    value_grad = jnp.einsum('bchk,bhkv->bchv', decayed.astype(jnp.float32), state_grad).astype(jnp.bfloat16).reshape(CORPUS_SPAN, FOCUS_GROUPS, HEAD_V)
    decayed_grad = jnp.einsum('bchv,bhkv->bchk', value_blocks, state_grad)
    key_grad = (decayed_grad * factor).astype(jnp.bfloat16).reshape(CORPUS_SPAN, QUERY_CHANNELS)
    combined_derivative = lax.optimization_barrier(jnp.sum(priors * jnp.exp(totals)[:, :, :, None] * state_grad, axis=3))
    moved_terms = decayed_grad * key_weight
    preceding_cumulation = jnp.cumsum(moved_terms, axis=1) - moved_terms
    preact_segments = persistence_scores.astype(jnp.float32).reshape(piece_ordinal, PIECE_PLACES, FOCUS_GROUPS, FEATURE_DIMS)
    retain_preact_derivative = ((combined_derivative[:, None] + preceding_cumulation) * jax.nn.sigmoid(-preact_segments) / toggle_smoothness).reshape(CORPUS_SPAN, QUERY_CHANNELS)

    def query_block(item):
        block_grad, block_state = item
        groups = jnp.einsum('chgv,hkgv->gchk', block_grad.reshape(PIECE_PLACES, FOCUS_GROUPS, N_TP, HV_PART), block_state.reshape(FOCUS_GROUPS, FEATURE_DIMS, N_TP, HV_PART)) * query_scale
        groups = lax.optimization_barrier(groups.astype(jnp.bfloat16))
        return lax.optimization_barrier(jnp.sum(groups.astype(jnp.float32), axis=0)).astype(jnp.bfloat16)
    query_grad = lax.map(query_block, (readout_blocks, states)).reshape(CORPUS_SPAN, QUERY_CHANNELS)
    return (stream_grad, gate_grad, up_grad, down_grad, proj_grad, query_grad, key_grad, retain_preact_derivative, value_grad, gate_input_grad)
```

```python
import functools

import jax
import jax.numpy as jnp
from jax import lax
from jax.experimental import pallas as pl
from jax.experimental.pallas import tpu as pltpu
from jax.sharding import PartitionSpec as P

PIECE_PLACES = 64
toggle_smoothness = 16.0
norm_eps = 1e-06

F32 = jnp.float32
BF16 = jnp.bfloat16
NT = (((1,), (1,)), ((), ()))
TN = (((0,), (0,)), ((), ()))
MIB = 1 << 20


def dot(a, b):
    return jnp.dot(a, b, preferred_element_type=F32)


def dot_nt(a, b):
    return lax.dot_general(a, b, NT, preferred_element_type=F32)


def dot_tn(a, b):
    return lax.dot_general(a, b, TN, preferred_element_type=F32)


def shape(dims, kind=BF16):
    return jax.ShapeDtypeStruct(dims, kind)


def call(body, name, where, operands, outs, scratch=(), flops=0, vmem=32):
    moved = sum(x.size * x.dtype.itemsize for x in (*operands, *outs))
    spec = pl.BlockSpec(memory_space=pltpu.VMEM)
    return pl.pallas_call(
        body,
        name=name,
        out_shape=tuple(outs),
        in_specs=[pl.BlockSpec(memory_space=pltpu.SMEM)] + [spec] * len(operands),
        out_specs=tuple([spec] * len(outs)),
        scratch_shapes=list(scratch),
        cost_estimate=pl.CostEstimate(
            flops=int(flops + moved), bytes_accessed=int(moved), transcendentals=0
        ),
        compiler_params=pltpu.CompilerParams(vmem_limit_bytes=vmem * MIB),
    )(where, *operands)


def swap(piece, axis, k):
    size = lax.axis_size(axis)
    return lax.ppermute(piece, axis, [(a, a ^ k) for a in range(size)])


def silu_slope(value):
    sigma = jax.nn.sigmoid(value)
    return sigma + value * sigma * (1.0 - sigma)


def prep_body(where, res_ref, adj_ref, gain_ref, *outs):
    tp = where[1]
    residual = res_ref[...].astype(F32)
    inv_rms = lax.rsqrt(jnp.mean(residual * residual, axis=1, keepdims=True) + norm_eps)
    moe = (residual * inv_rms * gain_ref[...]).astype(BF16)
    out = outs[0]
    parts = out.shape[0]
    width = out.shape[3]
    for q in range(parts):
        out[q ^ tp, 0] = moe[:, q * width : (q + 1) * width]
        out[q ^ tp, 1] = adj_ref[:, q * width : (q + 1) * width]


def dispatch_body(groups, local, cap, parts, where, ids_ref, share_ref, *refs):
    sp, tp = where[0], where[1]
    received = refs[:parts]
    x_out, c_out, pick_out, x_nat, c_nat = refs[parts:]
    own = x_nat.shape[1]
    width = x_nat.shape[2]
    tokens = parts * own
    for k in range(parts):
        x_nat[k ^ tp] = received[k][0].astype(F32)
        c_nat[k ^ tp] = received[k][1].astype(F32)
    xs = x_nat[...].reshape(tokens, width).astype(BF16)
    cs = c_nat[...].reshape(tokens, width).astype(BF16)
    total = groups * local
    padded = pick_out.shape[1]
    row = lax.broadcasted_iota(jnp.int32, (total, tokens), 0)
    expert = ((row // local) ^ sp) * local + row % local
    hit0 = ids_ref[0:1, :] == expert
    hit1 = ids_ref[1:2, :] == expert
    member = jnp.where(hit0 | hit1, 1.0, 0.0)
    share = jnp.where(hit0, share_ref[0:1, :], 0.0) + jnp.where(hit1, share_ref[1:2, :], 0.0)
    before = jnp.where(
        lax.broadcasted_iota(jnp.int32, (tokens, tokens), 0)
        < lax.broadcasted_iota(jnp.int32, (tokens, tokens), 1),
        1.0,
        0.0,
    ).astype(BF16)
    rank = dot(member.astype(BF16), before)
    place = lax.broadcasted_iota(jnp.int32, (total, padded, tokens), 1).astype(F32)
    pick = jnp.where(rank[:, None, :] == place, member[:, None, :], 0.0)
    scale = jnp.sum(pick * share[:, None, :], axis=2, keepdims=True).reshape(total * padded, 1)
    pick_out[...] = pick
    flat = pick.reshape(total * padded, tokens).astype(BF16)
    x_rows = dot(flat, xs)
    c_rows = dot(flat, cs) * scale
    for k in range(groups):
        for e in range(local):
            start = (k * local + e) * padded
            x_out[k, e] = x_rows[start : start + cap].astype(BF16)
            c_out[k, e] = c_rows[start : start + cap].astype(BF16)


def expert_in_body(parts, local, where, *refs):
    tp = where[1]
    xs = refs[:parts]
    wg, wu, g_out, u_out = refs[parts:]
    width = xs[0].shape[2]
    for e in range(local):
        for w, out in ((wg, g_out), (wu, u_out)):
            acc = None
            for k in range(parts):
                block = w[e, pl.ds(pl.multiple_of((k ^ tp) * width, width), width), :]
                term = dot(xs[k][e], block)
                acc = term if acc is None else acc + term
            out[e] = acc


def expert_mid_body(parts, local, where, *refs):
    tp = where[1]
    cs = refs[:parts]
    g_ref, u_ref, wg, wu, wd, hid_out, gp_out, up_out, part_out = refs[parts:]
    width = cs[0].shape[2]

    def at(k):
        return pl.ds(pl.multiple_of((k ^ tp) * width, width), width)

    for e in range(local):
        hg = None
        for k in range(parts):
            term = dot_nt(cs[k][e], wd[e, :, at(k)])
            hg = term if hg is None else hg + term
        g = g_ref[e]
        u = u_ref[e]
        sigma = jax.nn.sigmoid(g)
        act = g * sigma
        hid_out[e] = (act * u).astype(BF16)
        gp = (hg * u * (sigma + act * (1.0 - sigma))).astype(BF16)
        up = (hg * act).astype(BF16)
        gp_out[e] = gp
        up_out[e] = up
        for k in range(parts):
            value = dot_nt(gp, wg[e, at(k), :]) + dot_nt(up, wu[e, at(k), :])
            part_out[k, e] = value.astype(BF16)


def expert_grad_body(parts, local, where, *refs):
    tp = where[1]
    xs = refs[:parts]
    cs = refs[parts : 2 * parts]
    hid, gp, up, gg_out, ug_out, dg_out = refs[2 * parts :]
    width = cs[0].shape[2]
    for e in range(local):
        for k in range(parts):
            at = pl.ds(pl.multiple_of((k ^ tp) * width, width), width)
            gg_out[e, at, :] = dot_tn(xs[k][e], gp[e]).astype(BF16)
            ug_out[e, at, :] = dot_tn(xs[k][e], up[e]).astype(BF16)
            dg_out[e, :, at] = dot_tn(hid[e], cs[k][e]).astype(BF16)


def combine_body(groups, local, cap, where, pick_ref, *refs):
    rows = refs[:groups]
    out = refs[groups]
    acc = None
    for k in range(groups):
        for e in range(local):
            pick = pick_ref[k * local + e][0:cap].astype(BF16)
            term = dot_tn(pick, rows[k][e])
            acc = term if acc is None else acc + term
    out[...] = acc.astype(BF16)


def rows_body(parts, where, *refs):
    tp = where[1]
    received = refs[:parts]
    cot_out, unit_out, inv_out = refs[parts:]
    for k in range(parts):
        residual = received[k][0].astype(F32)
        inv_rms = lax.rsqrt(jnp.mean(residual * residual, axis=1, keepdims=True) + norm_eps)
        unit_out[k ^ tp] = residual * inv_rms
        inv_out[k ^ tp] = jnp.broadcast_to(inv_rms, inv_out.shape[1:])
        cot_out[k ^ tp] = received[k][1]


def mixer_body(
    heads,
    parts,
    where,
    look_ref,
    score_ref,
    shrink_ref,
    probe_ref,
    content_ref,
    valve_ref,
    memory_ref,
    gated_out,
    silu_out,
    slope_out,
    state_out,
    prior_out,
    qhat_out,
    q2_out,
    qc_out,
    deci_out,
    sc_out,
    e_out,
    factor_out,
    weight_out,
):
    tp = where[1]
    tokens, keys = look_ref.shape
    hk = keys // heads
    hv = content_ref.shape[1] // heads
    c = PIECE_PLACES
    blocks = tokens // c
    own = tokens // parts
    own_keys = keys // parts
    tri = jnp.where(
        lax.broadcasted_iota(jnp.int32, (c, c), 0) >= lax.broadcasted_iota(jnp.int32, (c, c), 1),
        1.0,
        0.0,
    )
    ones = jnp.ones((c, hv), F32)
    exact = lax.Precision.HIGHEST
    e_out[...] = jnp.zeros(e_out.shape, F32)
    for h in range(heads):
        ks = slice(h * hk, (h + 1) * hk)
        vs = slice(h * hv, (h + 1) * hv)
        score = score_ref[:, ks].astype(F32)
        log_sig = jnp.minimum(score, 0.0) - jnp.log1p(jnp.exp(-jnp.abs(score)))
        decay = log_sig / toggle_smoothness + shrink_ref[:, h : h + 1]
        state = memory_ref[h]
        prior_out[h] = state.astype(BF16)
        qh = probe_ref[:, ks].astype(F32) * (hk**-0.5)
        qhb = qh.astype(BF16)
        qhat_out[:, ks] = qhb
        gate = valve_ref[:, vs].astype(F32)
        sigma = jax.nn.sigmoid(gate)
        silu = gate * sigma
        slope = sigma + silu * (1.0 - sigma)
        silu_out[:, vs] = silu
        totals, kws, decs = [], [], []
        for b in range(blocks):
            bs = slice(b * c, (b + 1) * c)
            piece = decay[bs]
            cum = jnp.dot(tri, piece, precision=exact, preferred_element_type=F32)
            total = cum[c - 1 : c]
            factor = jnp.exp(total - cum)
            kw = look_ref[bs, ks].astype(F32) * factor
            factor_out[bs, ks] = factor
            weight_out[bs, ks] = kw
            dec = kw.astype(BF16)
            column = lax.dot_general(
                piece, ones, TN, precision=exact, preferred_element_type=F32
            )
            state = state * jnp.exp(column) + dot_tn(dec, content_ref[bs, vs])
            stb = state.astype(BF16)
            state_out[b, h] = stb
            readout = dot(qhb[bs], stb)
            slope_out[bs, vs] = readout * slope[bs]
            gated = (readout * silu[bs]).astype(BF16)
            for q in range(b * c // own, (b + 1) * c // own):
                gated_out[q ^ tp, :, vs] = gated[q * own - b * c : (q + 1) * own - b * c]
            e_out[b : b + 1, ks] = jnp.exp(total)
            totals.append(total)
            kws.append(kw)
            decs.append(dec)
        span = totals[0]
        for total in totals[1:]:
            span = span + total
        e_out[blocks : blocks + 1, ks] = span
        tail = jnp.zeros_like(totals[0])
        for b in reversed(range(blocks)):
            bs = slice(b * c, (b + 1) * c)
            deci_out[bs, ks] = (kws[b] * jnp.exp(tail)).astype(BF16)
            e_out[blocks + 1 + b : blocks + 2 + b, ks] = jnp.exp(tail)
            tail = tail + totals[b]
        lead = jnp.zeros_like(totals[0])
        for b in range(blocks):
            bs = slice(b * c, (b + 1) * c)
            if b > 0:
                lead = lead + totals[b]
            q2_out[bs, ks] = (qh[bs] * jnp.exp(lead)).astype(BF16)
            qc_out[bs, ks] = (qh[bs] * jnp.exp(lead + totals[0])).astype(BF16)
        for b in range(blocks):
            bs = slice(b * c, (b + 1) * c)
            gap = jnp.zeros_like(totals[0])
            for t in range(blocks):
                ts = slice(t * c, (t + 1) * c)
                if t < b:
                    sc_out[h, bs, ts] = jnp.zeros((c, c), BF16)
                    continue
                if t > b:
                    gap = gap + totals[t]
                left = (kws[b] * jnp.exp(gap)).astype(BF16)
                sc_out[h, bs, ts] = dot_nt(left, qhb[ts]).astype(BF16)


def stream_body(
    heads, groups, parts, where, *refs
):
    sp, tp = where[0], where[1]
    grads = refs[:parts]
    (
        cot_ref,
        unit_ref,
        inv_ref,
        gain_ref,
        w_ref,
        silu_ref,
        slope_ref,
        qc_ref,
        own_out,
        piece_out,
        rg_out,
        gig_out,
        carry_out,
        stream,
        rows,
    ) = refs[parts:]
    tokens, model = stream.shape
    width = model // parts
    own = tokens // parts
    inv = inv_ref[:, 0:1]

    def at(k):
        return pl.ds(pl.multiple_of((k ^ tp) * width, width), width)

    acc = None
    for k in range(parts):
        scaled = gain_ref[:, at(k)] * grads[k][...].astype(F32)
        term = jnp.sum(scaled * unit_ref[:, at(k)], axis=1, keepdims=True)
        acc = term if acc is None else acc + term
    mean = acc / model
    for k in range(parts):
        scaled = gain_ref[:, at(k)] * grads[k][...].astype(F32)
        value = cot_ref[:, at(k)].astype(F32) + inv * (scaled - unit_ref[:, at(k)] * mean)
        stream[:, at(k)] = value.astype(BF16)
    full = stream[...]
    for q in range(parts):
        rows[q] = full[q * own : (q + 1) * own].astype(F32)
    mine = rows[tp].astype(BF16)
    own_out[...] = mine
    cut = model // groups
    for q in range(groups):
        piece_out[q ^ sp] = mine[:, q * cut : (q + 1) * cut]
    gated_grad = dot(full, w_ref[...])
    rg = (gated_grad * silu_ref[...]).astype(BF16)
    rg_out[...] = rg
    gig_out[...] = (gated_grad * slope_ref[...]).astype(BF16)
    hk = qc_ref.shape[1] // heads
    hv = rg.shape[1] // heads
    slab = hk // groups
    for h in range(heads):
        carry = dot_tn(qc_ref[:, h * hk : (h + 1) * hk], rg[:, h * hv : (h + 1) * hv])
        carry = carry.astype(BF16)
        for q in range(groups):
            carry_out[q ^ sp, h] = carry[q * slab : (q + 1) * slab]


def local_body(
    heads,
    parts,
    where,
    rg_ref,
    content_ref,
    sc_ref,
    qhat_ref,
    q2_ref,
    state_ref,
    prior_ref,
    e_ref,
    value_out,
    dkey_out,
    total_out,
    query_out,
):
    tp = where[1]
    tokens, keys = qhat_ref.shape
    hk = keys // heads
    hv = content_ref.shape[1] // heads
    c = PIECE_PLACES
    blocks = tokens // c
    own_keys = keys // parts
    for h in range(heads):
        ks = slice(h * hk, (h + 1) * hk)
        vs = slice(h * hv, (h + 1) * hv)
        rg = rg_ref[:, vs]
        value_out[:, vs] = dot(sc_ref[h], rg)
        attn = dot_nt(content_ref[:, vs], rg).astype(BF16)
        for b in range(blocks):
            bs = slice(b * c, (b + 1) * c)
            if b == 0:
                later = q2_ref[:, ks]
            else:
                pieces = [qhat_ref[bs, ks]]
                ratio = None
                for t in range(b + 1, blocks):
                    ratio = e_ref[t : t + 1, ks] if ratio is None else ratio * e_ref[t : t + 1, ks]
                    q_t = qhat_ref[t * c : (t + 1) * c, ks].astype(F32) * ratio
                    pieces.append(q_t.astype(BF16))
                later = pieces[0] if len(pieces) == 1 else jnp.concatenate(pieces, axis=0)
            tail = slice(b * c, tokens)
            dkey_out[bs, ks] = dot(attn[bs, tail], later)
            prior = prior_ref[h] if b == 0 else state_ref[b - 1, h]
            cross = dot_nt(rg[tail], prior) * later.astype(F32)
            total_out[b : b + 1, ks] = e_ref[b : b + 1, ks] * jnp.sum(cross, axis=0, keepdims=True)
            query = dot_nt(rg[bs], state_ref[b, h]) * (hk**-0.5)
            lo, hi = h * hk, (h + 1) * hk
            for q in range(parts):
                a, z = max(lo, q * own_keys), min(hi, (q + 1) * own_keys)
                if a < z:
                    query_out[q ^ tp, bs, a - q * own_keys : z - q * own_keys] = query[
                        :, a - lo : z - lo
                    ].astype(BF16)


def scan_body(groups, where, d_ref, *refs):
    sp = where[0]
    pieces = refs[:groups]
    out = refs[groups]
    nat = refs[groups + 1]
    heads, slab, _ = pieces[0].shape
    for k in range(groups):
        nat[k ^ sp] = pieces[k][...]
    for h in range(heads):
        carried = jnp.zeros(pieces[0].shape[1:], F32)
        for s in reversed(range(groups)):
            out[s ^ sp, h] = carried.astype(BF16)
            decay = d_ref[h * slab : (h + 1) * slab, s : s + 1]
            carried = nat[s, h].astype(F32) + decay * carried


def tail_body(
    heads,
    groups,
    parts,
    where,
    content_ref,
    deci_ref,
    state_ref,
    prior_ref,
    e_ref,
    value_ref,
    dkey_ref,
    total_ref,
    *refs,
):
    sp, tp = where[0], where[1]
    pieces = refs[:groups]
    value_out, key_out, nat = refs[groups:]
    tokens, keys = deci_ref.shape
    hk = keys // heads
    hv = content_ref.shape[1] // heads
    c = PIECE_PLACES
    blocks = tokens // c
    own_keys = keys // parts
    for k in range(groups):
        nat[k ^ sp] = pieces[k][...]
    ones = jnp.ones((8, hv), BF16)
    for h in range(heads):
        ks = slice(h * hk, (h + 1) * hk)
        vs = slice(h * hv, (h + 1) * hv)
        incoming = nat[:, h].astype(F32).reshape(hk, hv)
        inb = incoming.astype(BF16)
        value_out[:, vs] = (value_ref[:, vs] + dot(deci_ref[:, ks], inb)).astype(BF16)
        reach = dot_nt(content_ref[:, vs], inb)
        lo, hi = h * hk, (h + 1) * hk
        sums = []
        for b in range(blocks):
            bs = slice(b * c, (b + 1) * c)
            after = e_ref[blocks + 1 + b : blocks + 2 + b, ks]
            dkey = (dkey_ref[bs, ks] + reach[bs] * after).astype(BF16)
            prior = prior_ref[h] if b == 0 else state_ref[b - 1, h]
            inner = dot_nt(ones, (prior.astype(F32) * incoming).astype(BF16))[0:1]
            sums.append(total_ref[b : b + 1, ks] + e_ref[b : b + 1, ks] * after * inner)
            for q in range(parts):
                a, z = max(lo, q * own_keys), min(hi, (q + 1) * own_keys)
                if a < z:
                    key_out[q ^ tp, bs, a - q * own_keys : z - q * own_keys] = dkey[
                        :, a - lo : z - lo
                    ]
        rows = jnp.concatenate(sums + [jnp.zeros((16 - blocks, hk), F32)], axis=0).astype(BF16)
        for q in range(parts):
            a, z = max(lo, q * own_keys), min(hi, (q + 1) * own_keys)
            if a < z:
                key_out[q ^ tp, tokens : tokens + 16, a - q * own_keys : z - q * own_keys] = rows[
                    :, a - lo : z - lo
                ]


def final_body(parts, where, factor_ref, weight_ref, score_ref, *refs):
    pieces = refs[:parts]
    key_out, retain_out = refs[parts:]
    tokens = key_out.shape[0]
    c = PIECE_PLACES
    total = pieces[0][...].astype(F32)
    for piece in pieces[1:]:
        total = total + piece[...].astype(F32)
    sums = total[:tokens]
    key_out[...] = (sums * factor_ref[...]).astype(BF16)
    moved = sums * weight_ref[...]
    gate = jax.nn.sigmoid(-score_ref[...].astype(F32)) / toggle_smoothness
    below = jnp.where(
        lax.broadcasted_iota(jnp.int32, (c, c), 0) > lax.broadcasted_iota(jnp.int32, (c, c), 1),
        1.0,
        0.0,
    )
    for b in range(tokens // c):
        bs = slice(b * c, (b + 1) * c)
        earlier = jnp.dot(
            below, moved[bs], precision=lax.Precision.HIGHEST, preferred_element_type=F32
        )
        retain_out[bs] = (total[tokens + b : tokens + b + 1] + earlier) * gate[bs]


def on_device(
    residual_signal,
    prelayer_scaling_factor,
    result_adjoint,
    chosen_specialist_ids,
    dispatch_shares,
    specialist_valve_matrix,
    specialist_widen_matrix,
    specialist_shrink_matrix,
    probe_vectors,
    lookup_vectors,
    persistence_scores,
    group_additional_shrinkage,
    content_vectors,
    result_valve_scores,
    stored_opening_memory,
    result_mapping_matrix,
):
    part = functools.partial
    parts = lax.axis_size("tp")
    groups = lax.axis_size("sp")
    sp, tp = lax.axis_index("sp"), lax.axis_index("tp")
    where = jnp.stack([sp, tp]).astype(jnp.int32)
    own, model = residual_signal.shape
    width = model // parts
    tokens = own * parts
    top = chosen_specialist_ids.shape[1]
    local = specialist_valve_matrix.shape[0]
    hidden = specialist_valve_matrix.shape[2]
    total = local * groups
    assigned = tokens * top
    cap = assigned // total + assigned // (4 * total)
    padded = -(-cap // 8) * 8
    gain = prelayer_scaling_factor.reshape(1, model)
    heads = group_additional_shrinkage.shape[1]
    keys = probe_vectors.shape[1]
    hk = keys // heads
    hv = content_vectors.shape[2]
    blocks = tokens // PIECE_PLACES
    own_keys = keys // parts
    slab = hk // groups
    cut = model // groups

    (send,) = call(
        prep_body,
        "prep",
        where,
        (residual_signal, result_adjoint, gain),
        (shape((parts, 2, own, width)),),
    )
    received = [send[0]] + [swap(send[k], "tp", k) for k in range(1, parts)]
    x_send, c_send, pick = call(
        part(dispatch_body, groups, local, cap, parts),
        "dispatch",
        where,
        (chosen_specialist_ids.T, dispatch_shares.T, *received),
        (
            shape((groups, local, cap, width)),
            shape((groups, local, cap, width)),
            shape((total, padded, tokens), F32),
        ),
        scratch=(
            pltpu.VMEM((parts, own, width), F32),
            pltpu.VMEM((parts, own, width), F32),
        ),
    )

    def to_experts(send):
        got = [send[0]] + [swap(send[k], "sp", k) for k in range(1, groups)]
        mine = jnp.concatenate(got, axis=1)
        return [mine] + [swap(mine, "tp", k) for k in range(1, parts)]

    xs = to_experts(x_send)
    cs = to_experts(c_send)
    rows = groups * cap
    pre_gate, pre_up = call(
        part(expert_in_body, parts, local),
        "expert_in",
        where,
        (*xs, specialist_valve_matrix, specialist_widen_matrix),
        (shape((local, rows, hidden), F32), shape((local, rows, hidden), F32)),
        flops=4 * rows * model * hidden,
    )
    hid, gp, up, partial_value = call(
        part(expert_mid_body, parts, local),
        "expert_mid",
        where,
        (
            *cs,
            pre_gate,
            pre_up,
            specialist_valve_matrix,
            specialist_widen_matrix,
            specialist_shrink_matrix,
        ),
        (
            shape((local, rows, hidden)),
            shape((local, rows, hidden)),
            shape((local, rows, hidden)),
            shape((parts, local, rows, width)),
        ),
        flops=6 * rows * model * hidden,
    )
    gate_grad, up_grad, down_grad = call(
        part(expert_grad_body, parts, local),
        "expert_grad",
        where,
        (*xs, *cs, hid, gp, up),
        (
            shape((local, model, hidden)),
            shape((local, model, hidden)),
            shape((local, hidden, model)),
        ),
        flops=6 * rows * model * hidden,
    )
    summed = partial_value[0].astype(F32)
    for k in range(1, parts):
        summed = summed + swap(partial_value[k], "tp", k).astype(F32)
    summed = summed.astype(BF16).reshape(local, groups, cap, width)
    back = [summed[:, 0]] + [swap(summed[:, k], "sp", k) for k in range(1, groups)]
    (grad_columns,) = call(
        part(combine_body, groups, local, cap),
        "combine",
        where,
        (pick, *back),
        (shape((tokens, width)),),
    )
    grads = [grad_columns] + [swap(grad_columns, "tp", k) for k in range(1, parts)]

    paired = jnp.stack([residual_signal, result_adjoint])
    span_rows = [paired] + [swap(paired, "tp", k) for k in range(1, parts)]
    cot, unit, inv = call(
        part(rows_body, parts),
        "rows",
        where,
        span_rows,
        (
            shape((parts, own, model)),
            shape((parts, own, model), F32),
            shape((parts, own, 128), F32),
        ),
    )
    cot = cot.reshape(tokens, model)
    unit = unit.reshape(tokens, model)
    inv = inv.reshape(tokens, 128)

    content = content_vectors.reshape(tokens, heads * hv)
    valve = result_valve_scores.reshape(tokens, heads * hv)
    (
        gated,
        silu,
        slope,
        states,
        prior,
        qhat,
        q2,
        qc,
        deci,
        sc,
        e_rows,
        factor,
        weight,
    ) = call(
        part(mixer_body, heads, parts),
        "mixer",
        where,
        (
            lookup_vectors,
            persistence_scores,
            group_additional_shrinkage,
            probe_vectors,
            content,
            valve,
            stored_opening_memory[0],
        ),
        (
            shape((parts, own, heads * hv)),
            shape((tokens, heads * hv), F32),
            shape((tokens, heads * hv), F32),
            shape((blocks, heads, hk, hv)),
            shape((heads, hk, hv)),
            shape((tokens, keys)),
            shape((tokens, keys)),
            shape((tokens, keys)),
            shape((tokens, keys)),
            shape((heads, tokens, tokens)),
            shape((-(-(2 * blocks + 1) // 8) * 8, keys), F32),
            shape((tokens, keys), F32),
            shape((tokens, keys), F32),
        ),
        flops=10 * tokens * keys * hv,
    )
    span_logs = lax.all_gather(e_rows[blocks], "sp", axis=0)
    decays = jnp.exp(
        lax.dynamic_slice_in_dim(span_logs.reshape(groups, heads, hk), sp * slab, slab, 2)
    )
    decays = decays.reshape(groups, heads * slab).T

    def own_columns(tensor):
        return lax.dynamic_slice_in_dim(tensor, tp * own_keys, own_keys, 1)

    factor_own = own_columns(factor)
    weight_own = own_columns(weight)
    score_own = own_columns(persistence_scores)

    same = [k for k in range(2, groups, 2)]
    held = jnp.stack([gated] + [swap(gated, "sp", k) for k in same])
    other = swap(held, "sp", 1)
    gated_all = jnp.stack([held, other], axis=1).reshape(groups * tokens, heads * hv)

    mapping = result_mapping_matrix.reshape(model, heads * hv)
    stream_own, stream_pieces, rg, gate_input_grad, carry = call(
        part(stream_body, heads, groups, parts),
        "stream",
        where,
        (*grads, cot, unit, inv, gain, mapping, silu, slope, qc),
        (
            shape((own, model)),
            shape((groups, own, cut)),
            shape((tokens, heads * hv)),
            shape((tokens, heads * hv)),
            shape((groups, heads, slab, hv)),
        ),
        scratch=(pltpu.VMEM((tokens, model), BF16), pltpu.VMEM((parts, own, model), F32)),
        flops=2 * tokens * model * heads * hv,
    )
    carries = [carry[0]] + [swap(carry[k], "sp", k) for k in range(1, groups)]
    value_local, dkey_local, total_local, query_parts = call(
        part(local_body, heads, parts),
        "local",
        where,
        (rg, content, sc, qhat, q2, states, prior, e_rows),
        (
            shape((tokens, heads * hv), F32),
            shape((tokens, keys), F32),
            shape((8, keys), F32),
            shape((parts, tokens, own_keys)),
        ),
        flops=8 * tokens * keys * hv,
    )
    (incoming,) = call(
        part(scan_body, groups),
        "scan",
        where,
        (decays, *carries),
        (shape((groups, heads, slab, hv)),),
        scratch=(pltpu.VMEM((groups, heads, slab, hv), BF16),),
    )
    arrived = [incoming[0]] + [swap(incoming[k], "sp", k) for k in range(1, groups)]
    value_grad, key_parts = call(
        part(tail_body, heads, groups, parts),
        "tail",
        where,
        (content, deci, states, prior, e_rows, value_local, dkey_local, total_local, *arrived),
        (shape((tokens, heads * hv)), shape((parts, tokens + 16, own_keys))),
        scratch=(pltpu.VMEM((groups, heads, slab, hv), BF16),),
        flops=4 * tokens * keys * hv,
    )
    key_pieces = [key_parts[0]] + [swap(key_parts[k], "tp", k) for k in range(1, parts)]
    key_grad, retain = call(
        part(final_body, parts),
        "final",
        where,
        (factor_own, weight_own, score_own, *key_pieces),
        (shape((tokens, own_keys)), shape((tokens, own_keys), F32)),
    )
    query_sum = query_parts[0].astype(F32)
    for k in range(1, parts):
        query_sum = query_sum + swap(query_parts[k], "tp", k).astype(F32)
    query_grad = query_sum.astype(BF16)

    stream_rows = jnp.stack(
        [stream_pieces[0]] + [swap(stream_pieces[k], "sp", k) for k in range(1, groups)]
    )
    stream_all = jnp.stack(
        [stream_rows] + [swap(stream_rows, "tp", k) for k in range(1, parts)], axis=1
    ).reshape(groups * tokens, cut)
    proj_grad = dot_tn(stream_all, gated_all).reshape(cut, heads, hv)

    return (
        stream_own,
        gate_grad,
        up_grad,
        down_grad,
        proj_grad,
        query_grad,
        key_grad,
        retain,
        value_grad.reshape(tokens, heads, hv),
        gate_input_grad.reshape(tokens, heads, hv),
    )


def solution(mesh):
    return jax.shard_map(
        on_device,
        mesh=mesh,
        in_specs=(
            P(("sp", "tp"), None),
            P(),
            P(("sp", "tp"), None),
            P("sp", None),
            P("sp", None),
            P("sp", None, "tp"),
            P("sp", None, "tp"),
            P("sp", "tp", None),
            P("sp", None),
            P("sp", None),
            P("sp", None),
            P("sp", None),
            P("sp", None, "tp"),
            P("sp", None, "tp"),
            P("sp", None, None, "tp"),
            P(None, None, "tp"),
        ),
        out_specs=(
            P(("sp", "tp"), None),
            P("sp", None, "tp"),
            P("sp", None, "tp"),
            P("sp", "tp", None),
            P("sp", None, "tp"),
            P("sp", "tp"),
            P("sp", "tp"),
            P("sp", "tp"),
            P("sp", None, "tp"),
            P("sp", None, "tp"),
        ),
        check_vma=False,
    )
```
